32 devices in a mesh: sp: 4 (over z), dp: 8 (over y, x, core).
Axes of the slice: x: 2, y: 2, z: 4, core: 2. Of those that a mesh axis runs over, the one named last changes fastest.
Arguments:
- queries: bfloat16 [8, 768, 6144], P('dp', None, 'sp'), may hold values from -64 to 64
- out_grad: bfloat16 [8, 768, 4096], P('dp', None, 'sp'), may hold values from -6 to 6
- latent: bfloat16 [8, 768, 512], P('dp'), may hold values from -6 to 6
- rope_key: bfloat16 [8, 768, 64], P('dp'), may hold values from -6 to 6
- kv_gain: float32 [512], replicated, may hold values from 0.1 to 1.9
- key_up: bfloat16 [512, 4096], P('dp', 'sp'), may hold values from -0.25 to 0.25
- value_up: bfloat16 [512, 4096], P('dp', 'sp'), may hold values from -0.25 to 0.25
Outputs:
- query_grad: bfloat16 [8, 768, 6144], P('dp', None, 'sp')
- latent_grad: bfloat16 [8, 768, 512], P('dp')
- rope_key_grad: bfloat16 [8, 768, 64], P('dp')
- key_up_grad: float32 [512, 4096], P('dp', 'sp')
- value_up_grad: float32 [512, 4096], P('dp', 'sp')
The draws below stay inside these ranges and needn't reach their ends.
All inputs are finite; a program needn't handle non-finite values.
Results may differ from the reference program's by a relative error of at most 0.019.
The reference program's roundings to bfloat16 on the way count: a program that leaves them out, or rounds other values in their place, can miss the bound.
Values may be sent and summed in bfloat16 or wider, within the bound.
A program may use at most 64 MiB of HBM per device.

```python
import jax
import jax.numpy as jnp
from jax import lax

HEADS = 32
NOPE_DIM = 128
ROPE_DIM = 64
VALUE_DIM = 128
LATENT = 512
SEQ_LEN = 768
BATCH = 8
TOKENS = 6144
N_SP = 4


def draw_queries(key, part):
    shape = (BATCH, SEQ_LEN, HEADS * (NOPE_DIM + ROPE_DIM))
    base_key = jax.random.fold_in(key, 0)
    entries = jnp.clip(jax.random.normal(base_key, shape, jnp.float32), -6.0, 6.0)
    return entries.astype(jnp.bfloat16)


def shard_levels(stream_key, dims, pieces, smallest, high):
    level, own = 1.0, jax.random.fold_in(stream_key, 6)
    for dim, blocks in pieces:
        steps = jnp.exp(jax.random.uniform(jax.random.fold_in(own, dim), (blocks,), jnp.float32, smallest / len(pieces), high / len(pieces)))
        level = level * jnp.repeat(steps, dims[dim] // blocks).reshape([-1 if axis == dim else 1 for axis in range(len(dims))])
    return level


def normal_values(own_key, extent, scale, limit, shards=(), kind=jnp.bfloat16):
    result = jax.random.normal(own_key, extent, jnp.float32) * scale
    if len(shards) > 0:
        result = shard_levels(own_key, extent, shards, -0.22, 0.18) * result
    return jnp.clip(result, min=-limit, max=limit).astype(kind)


def setup_inputs(seed: int = 0) -> dict:
    splits = jax.random.split(jax.random.key(seed), 8)
    queries = draw_queries(jax.random.fold_in(splits[7], 71), 0)
    out_grad = normal_values(splits[1], (BATCH, SEQ_LEN, HEADS * VALUE_DIM), 1.0, 6.0, ((0, 8), (2, 4)))
    latent = normal_values(splits[2], (BATCH, SEQ_LEN, LATENT), 1.0, 6.0, ((0, 8),))
    rope_key = normal_values(splits[3], (BATCH, SEQ_LEN, ROPE_DIM), 1.0, 6.0, ((0, 8),))
    kv_gain = jnp.clip(1.0 + 0.18 * jax.random.normal(splits[4], (LATENT,), jnp.float32), 0.1, 1.9)
    key_up = normal_values(splits[5], (LATENT, HEADS * NOPE_DIM), LATENT ** -0.5, 0.25, ((0, 8), (1, 4)))
    value_up = normal_values(splits[6], (LATENT, HEADS * VALUE_DIM), LATENT ** -0.5, 0.25, ((0, 8), (1, 4)))
    return {"queries": queries, "out_grad": out_grad, "latent": latent, "rope_key": rope_key, "kv_gain": kv_gain, "key_up": key_up, "value_up": value_up}


norm_eps = 1e-06
rope_theta = 10000.0

def rope_tables(length, width):
    half_width = width // 2
    frequency = rope_theta ** (-(jnp.arange(half_width, dtype=jnp.float32) * 2.0 / width))
    position = jnp.arange(length, dtype=jnp.int32).astype(jnp.float32)
    angles = position[:, None] * frequency[None, :]
    return (jnp.cos(angles), jnp.sin(angles))

def rotate(tensor, cosine, sine_table):
    half_width = tensor.shape[-1] // 2
    first_half = tensor[..., :half_width]
    second = tensor[..., half_width:]
    return jnp.concatenate([first_half * cosine - second * sine_table, second * cosine + first_half * sine_table], axis=-1)

def unrotate(upstream, cosine, sine_table):
    half_width = upstream.shape[-1] // 2
    first_half = upstream[..., :half_width]
    second = upstream[..., half_width:]
    return jnp.concatenate([first_half * cosine + second * sine_table, second * cosine - first_half * sine_table], axis=-1)

def head_backward(query_used, key_used, head_value, head_grad, score_scale):
    length = query_used.shape[0]
    scores = jnp.dot(query_used, key_used.T, preferred_element_type=jnp.float32) * score_scale
    causal = lax.broadcasted_iota(jnp.int32, (length, length), 0) >= lax.broadcasted_iota(jnp.int32, (length, length), 1)
    scores = jnp.where(causal, scores, -jnp.inf)
    row_top = lax.optimization_barrier(jnp.max(scores, axis=1, keepdims=True))
    weights = jnp.exp(scores - row_top)
    probs = weights / lax.optimization_barrier(jnp.sum(weights, axis=1, keepdims=True))
    probs_low = probs.astype(jnp.bfloat16)
    value_grad = jnp.dot(probs_low.T, head_grad, preferred_element_type=jnp.float32).astype(jnp.bfloat16)
    prob_grad = jnp.dot(head_grad, head_value.T, preferred_element_type=jnp.float32)
    center = lax.optimization_barrier(jnp.sum(probs * prob_grad, axis=1, keepdims=True))
    score_grad = (probs * (prob_grad - center) * score_scale).astype(jnp.bfloat16)
    query_grad = jnp.dot(score_grad, key_used, preferred_element_type=jnp.float32)
    key_grad = jnp.dot(score_grad.T, query_used, preferred_element_type=jnp.float32)
    return (query_grad, key_grad, value_grad)

def attend(queries, head_grads, keys, values, key_rot, cosine, sine_table):
    length = queries.shape[0]
    head_count = head_grads.shape[1] // VALUE_DIM
    qk_width = NOPE_DIM + ROPE_DIM
    query_heads = queries.reshape(length, head_count, qk_width)
    rotated = rotate(query_heads[:, :, NOPE_DIM:].astype(jnp.float32), cosine[:, None, :], sine_table[:, None, :]).astype(jnp.bfloat16)
    query_used = jnp.concatenate([query_heads[:, :, :NOPE_DIM], rotated], axis=-1).transpose(1, 0, 2)
    key_heads = keys.reshape(length, head_count, NOPE_DIM).transpose(1, 0, 2)
    key_used = jnp.concatenate([key_heads, jnp.broadcast_to(key_rot[None], (head_count, length, ROPE_DIM))], axis=-1)
    value_heads = values.reshape(length, head_count, VALUE_DIM).transpose(1, 0, 2)
    grad_heads = head_grads.reshape(length, head_count, VALUE_DIM).transpose(1, 0, 2)
    score_scale = qk_width ** (-0.5)
    query_part, key_part, value_part = lax.map(lambda items: head_backward(items[0], items[1], items[2], items[3], score_scale), (query_used, key_used, value_heads, grad_heads))
    query_rot_grad = unrotate(query_part[:, :, NOPE_DIM:], cosine[None], sine_table[None])
    query_grad = jnp.concatenate([query_part[:, :, :NOPE_DIM], query_rot_grad], axis=-1).astype(jnp.bfloat16)
    query_grad = query_grad.transpose(1, 0, 2).reshape(length, head_count * qk_width)
    key_plain_grad = key_part[:, :, :NOPE_DIM].astype(jnp.bfloat16).transpose(1, 0, 2).reshape(length, head_count * NOPE_DIM)
    key_rot_grad = lax.optimization_barrier(jnp.sum(key_part[:, :, NOPE_DIM:], axis=0))
    value_grad = value_part.transpose(1, 0, 2).reshape(length, head_count * VALUE_DIM)
    return (query_grad, key_plain_grad, key_rot_grad, value_grad)

def finish(comp_total, rot_total, raw_latent, inverse, kv_gain, cosine, sine_table):
    mixed = comp_total * kv_gain
    spread = lax.optimization_barrier(jnp.mean(raw_latent * mixed, axis=-1, keepdims=True))
    latent_grad = (inverse * mixed - raw_latent * inverse ** 3 * spread).astype(jnp.bfloat16)
    rope_grad = unrotate(rot_total, cosine, sine_table).astype(jnp.bfloat16)
    return (latent_grad, rope_grad)

def reference(queries, out_grad, latent, rope_key, kv_gain, key_up, value_up):
    qk_width = NOPE_DIM + ROPE_DIM
    group = HEADS // N_SP
    cosine, sine_table = rope_tables(SEQ_LEN, ROPE_DIM)

    def one_sequence(totals, inputs):
        key_total, value_total = totals
        seq_queries, seq_grad, seq_latent, seq_rope = inputs
        raw_latent = seq_latent.astype(jnp.float32)
        inverse = lax.rsqrt(lax.optimization_barrier(jnp.mean(raw_latent * raw_latent, axis=-1, keepdims=True)) + norm_eps)
        compressed = (raw_latent * inverse * kv_gain).astype(jnp.bfloat16)
        key_rot = rotate(seq_rope.astype(jnp.float32), cosine, sine_table).astype(jnp.bfloat16)
        keys = jnp.dot(compressed, key_up, preferred_element_type=jnp.float32).astype(jnp.bfloat16)
        values = jnp.dot(compressed, value_up, preferred_element_type=jnp.float32).astype(jnp.bfloat16)

        def per_group(index):
            query_cols = lax.dynamic_slice_in_dim(seq_queries, index * (group * qk_width), group * qk_width, 1)
            grad_cols = lax.dynamic_slice_in_dim(seq_grad, index * (group * VALUE_DIM), group * VALUE_DIM, 1)
            key_cols = lax.dynamic_slice_in_dim(keys, index * (group * NOPE_DIM), group * NOPE_DIM, 1)
            value_cols = lax.dynamic_slice_in_dim(values, index * (group * VALUE_DIM), group * VALUE_DIM, 1)
            key_weight = lax.dynamic_slice_in_dim(key_up, index * (group * NOPE_DIM), group * NOPE_DIM, 1)
            value_weight = lax.dynamic_slice_in_dim(value_up, index * (group * VALUE_DIM), group * VALUE_DIM, 1)
            query_grad, key_plain_grad, key_rot_grad, value_grad = attend(query_cols, grad_cols, key_cols, value_cols, key_rot, cosine, sine_table)
            comp_part = jnp.dot(key_plain_grad, key_weight.T, preferred_element_type=jnp.float32) + jnp.dot(value_grad, value_weight.T, preferred_element_type=jnp.float32)
            return (query_grad, key_plain_grad, value_grad, comp_part, key_rot_grad)
        query_groups, key_groups, value_groups, comp_parts, rot_parts = lax.map(per_group, jnp.arange(N_SP, dtype=jnp.int32))
        query_grad = query_groups.transpose(1, 0, 2).reshape(SEQ_LEN, HEADS * qk_width)
        key_plain_all = key_groups.transpose(1, 0, 2).reshape(SEQ_LEN, HEADS * NOPE_DIM)
        value_all = value_groups.transpose(1, 0, 2).reshape(SEQ_LEN, HEADS * VALUE_DIM)
        comp_low = lax.optimization_barrier(comp_parts.astype(jnp.bfloat16))
        rot_low = lax.optimization_barrier(rot_parts.astype(jnp.bfloat16))
        comp_total = lax.optimization_barrier(jnp.sum(comp_low.astype(jnp.float32), axis=0))
        rot_total = lax.optimization_barrier(jnp.sum(rot_low.astype(jnp.float32), axis=0))
        latent_grad, rope_grad = finish(comp_total, rot_total, raw_latent, inverse, kv_gain, cosine, sine_table)
        contract = (((0,), (0,)), ((), ()))
        key_total = key_total + lax.dot_general(compressed, key_plain_all, contract, preferred_element_type=jnp.float32)
        value_total = value_total + lax.dot_general(compressed, value_all, contract, preferred_element_type=jnp.float32)
        return ((key_total, value_total), (query_grad, latent_grad, rope_grad))
    start_totals = (jnp.zeros((LATENT, HEADS * NOPE_DIM), jnp.float32), jnp.zeros((LATENT, HEADS * VALUE_DIM), jnp.float32))
    totals, outputs = lax.scan(one_sequence, start_totals, (queries, out_grad, latent, rope_key))
    grad_scale = float(TOKENS) ** (-0.5)
    return (outputs[0], outputs[1], outputs[2], totals[0] * grad_scale, totals[1] * grad_scale)
```

```python
import functools

import jax
import jax.numpy as jnp
import numpy as np
from jax import lax
from jax.experimental import pallas as pl
from jax.experimental.pallas import tpu as pltpu
from jax.sharding import PartitionSpec as P

NOPE_DIM = 128
ROPE_DIM = 64
VALUE_DIM = 128
QK = NOPE_DIM + ROPE_DIM
LOG2E = 1.4426950408889634

norm_eps = 1e-06
rope_theta = 10000.0

NT = (((1,), (1,)), ((), ()))


def rope_tables(length):
    half = ROPE_DIM // 2
    frequency = np.float32(rope_theta) ** (-(np.arange(half, dtype=np.float32) * np.float32(2.0 / ROPE_DIM)))
    angles = np.arange(length, dtype=np.float32)[:, None] * frequency.astype(np.float32)[None, :]
    return np.cos(angles).astype(np.float32), np.sin(angles).astype(np.float32)


def dot(a, b):
    return jnp.dot(a, b, preferred_element_type=jnp.float32)


def dot_nt(a, b):
    return lax.dot_general(a, b, NT, preferred_element_type=jnp.float32)


def swap_halves(x):
    lane = lax.broadcasted_iota(jnp.int32, x.shape, 1)
    return jnp.where(lane % ROPE_DIM < ROPE_DIM // 2, pltpu.roll(x, 96, 1), pltpu.roll(x, 32, 1))


def attention_kernel(
    block, grad_scale,
    latent_ref, rope_ref, gain_ref, cos_ref, sin_ref, cos_t_ref, sin_t_ref,
    q_ref, do_ref, wk_ref, wv_ref,
    dq_ref, dw_ref, part_ref, rot_ref,
    comp, comp_t, krot, krot_t, ku, kt, vals, qu, pt, dst, dkv, acc, rot_acc,
):
    step = pl.program_id(0)
    length = q_ref.shape[0]
    tiles = length // block
    scale = QK ** (-0.5)

    @pl.when(step == 0)
    def _():
        raw = latent_ref[...].astype(jnp.float32)
        inverse = lax.rsqrt(jnp.mean(raw * raw, axis=-1, keepdims=True) + norm_eps)
        normed = raw * inverse * gain_ref[...]
        comp[...] = normed.astype(jnp.bfloat16)
        comp_t[...] = normed.T.astype(jnp.bfloat16)
        rope = rope_ref[...].astype(jnp.float32)
        wide = jnp.concatenate([rope, rope], axis=1)
        turned = wide * cos_ref[...] + swap_halves(wide) * sin_ref[...]
        krot[...] = turned.astype(jnp.bfloat16)
        krot_t[...] = turned.T.astype(jnp.bfloat16)
        acc[...] = jnp.zeros_like(acc)
        rot_acc[...] = jnp.zeros_like(rot_acc)

    keys = dot(comp[...], wk_ref[...])
    keys_t = keys.T.astype(jnp.bfloat16)
    keys = keys.astype(jnp.bfloat16)
    vals[...] = dot(comp[...], wv_ref[...]).astype(jnp.bfloat16)
    for h in range(2):
        ku[h, :, :NOPE_DIM] = keys[:, h * NOPE_DIM:(h + 1) * NOPE_DIM]
        ku[h, :, NOPE_DIM:] = krot[:, :ROPE_DIM]
        kt[h, :NOPE_DIM, :] = keys_t[h * NOPE_DIM:(h + 1) * NOPE_DIM, :]
        kt[h, NOPE_DIM:, :] = krot_t[:ROPE_DIM, :]

    mid = q_ref[:, 128:256].astype(jnp.float32)
    last = q_ref[:, 256:384].astype(jnp.float32)
    low = lax.broadcasted_iota(jnp.int32, mid.shape, 1) < 64
    plain = jnp.where(low, pltpu.roll(mid, 64, 1), pltpu.roll(last, 64, 1))
    rope = jnp.where(low, mid, last)
    turned = rope * cos_ref[...] + swap_halves(rope) * sin_ref[...]
    qu[0, :, :NOPE_DIM] = q_ref[:, :128]
    qu[0, :, NOPE_DIM:] = turned[:, :ROPE_DIM].astype(jnp.bfloat16)
    qu[1, :, :NOPE_DIM] = plain.astype(jnp.bfloat16)
    qu[1, :, NOPE_DIM:] = pltpu.roll(turned, 64, 1)[:, :ROPE_DIM].astype(jnp.bfloat16)

    for i in range(tiles):
        rows = slice(i * block, (i + 1) * block)
        n = (i + 1) * block
        parts = []
        for h in range(2):
            cols = slice(h * VALUE_DIM, (h + 1) * VALUE_DIM)
            scores = dot_nt(ku[h, :n, :], qu[h, rows, :])
            key_at = lax.broadcasted_iota(jnp.int32, (block, block), 0)
            query_at = lax.broadcasted_iota(jnp.int32, (block, block), 1)
            diag = jnp.where(key_at <= query_at, scores[n - block:], -jnp.inf)
            scores = diag if i == 0 else jnp.concatenate([scores[:n - block], diag], axis=0)
            top = jnp.max(scores, axis=0, keepdims=True)
            e = jnp.exp2((scores - top) * (scale * LOG2E))
            r = 1.0 / jnp.sum(e, axis=0, keepdims=True)
            prob_grad = dot_nt(vals[:n, cols], do_ref[rows, cols])
            center = jnp.sum(e * prob_grad, axis=0, keepdims=True) * r
            pt[h, :n, rows] = (e * r).astype(jnp.bfloat16)
            ds = (e * (r * scale) * (prob_grad - center)).astype(jnp.bfloat16)
            dst[h, :n, rows] = ds
            g = dot(kt[h, :, :n], ds)
            a = g[NOPE_DIM:NOPE_DIM + 32]
            b = g[NOPE_DIM + 32:]
            c, s = cos_t_ref[:, rows], sin_t_ref[:, rows]
            parts += [g[:NOPE_DIM], a * c + b * s, b * c - a * s]
        dq_ref[rows, :] = jnp.concatenate(parts, axis=0).T.astype(jnp.bfloat16)

    for h in range(2):
        for j in range(tiles):
            rows = slice(j * block, (j + 1) * block)
            cols = slice(h * VALUE_DIM, (h + 1) * VALUE_DIM)
            dv = dot(pt[h, rows, j * block:], do_ref[j * block:, cols])
            dk = dot(dst[h, rows, j * block:], qu[h, j * block:, :])
            dkv[rows, h * NOPE_DIM:(h + 1) * NOPE_DIM] = dk[:, :NOPE_DIM].astype(jnp.bfloat16)
            dkv[rows, (2 + h) * 128:(3 + h) * 128] = dv.astype(jnp.bfloat16)
            rot_acc[rows, :] += dk[:, NOPE_DIM:]

    dw = dot(comp_t[...], dkv[...]) * grad_scale
    dw_ref[0] = dw[:, :256].astype(dw_ref.dtype)
    dw_ref[1] = dw[:, 256:].astype(dw_ref.dtype)
    acc[...] += dot_nt(dkv[:, :256], wk_ref[...]) + dot_nt(dkv[:, 256:], wv_ref[...])

    @pl.when(step == pl.num_programs(0) - 1)
    def _():
        part_ref[...] = acc[...].astype(jnp.bfloat16)
        rot_ref[...] = rot_acc[...].astype(jnp.bfloat16)


def attention(queries, out_grad, latent, rope_key, kv_gain, key_whole, value_whole, grad_scale):
    length = queries.shape[0]
    width = latent.shape[1]
    pairs = key_whole.shape[1] // 256
    block = 256
    cosine, sine = rope_tables(length)
    cos_wide = np.tile(cosine, (1, 4))
    sin_wide = np.concatenate([-sine, sine, -sine, sine], axis=1)
    bf, f32 = jnp.bfloat16, jnp.float32
    whole = lambda shape: pl.BlockSpec(shape, lambda p: (0,) * len(shape))
    column = lambda rows, cols: pl.BlockSpec((rows, cols), lambda p: (0, p))
    return pl.pallas_call(
        functools.partial(attention_kernel, block, grad_scale),
        grid=(pairs,),
        in_specs=[
            whole((length, width)), whole((length, ROPE_DIM)), whole((1, width)),
            whole((length, 128)), whole((length, 128)),
            whole((32, length)), whole((32, length)),
            column(length, 2 * QK), column(length, 256), column(width, 256), column(width, 256),
        ],
        out_specs=[
            column(length, 2 * QK),
            pl.BlockSpec((2, width, 256), lambda p: (0, 0, p)),
            whole((length, width)), whole((length, ROPE_DIM)),
        ],
        out_shape=[
            jax.ShapeDtypeStruct(queries.shape, bf),
            jax.ShapeDtypeStruct((2, width, key_whole.shape[1]), bf),
            jax.ShapeDtypeStruct((length, width), bf),
            jax.ShapeDtypeStruct((length, ROPE_DIM), bf),
        ],
        scratch_shapes=[
            pltpu.VMEM((length, width), bf), pltpu.VMEM((width, length), bf),
            pltpu.VMEM((length, 128), bf), pltpu.VMEM((128, length), bf),
            pltpu.VMEM((2, length, QK), bf), pltpu.VMEM((2, QK, length), bf),
            pltpu.VMEM((length, 256), bf), pltpu.VMEM((2, length, QK), bf),
            pltpu.VMEM((2, length, length), bf), pltpu.VMEM((2, length, length), bf),
            pltpu.VMEM((length, 512), bf),
            pltpu.VMEM((length, width), f32), pltpu.VMEM((length, ROPE_DIM), f32),
        ],
        compiler_params=pltpu.CompilerParams(
            dimension_semantics=("arbitrary",), vmem_limit_bytes=48 * 1024 * 1024
        ),
        cost_estimate=pl.CostEstimate(flops=10_000_000_000, bytes_accessed=12_000_000, transcendentals=4_000_000),
        name="attention_backward",
    )(
        latent, rope_key, kv_gain.reshape(1, -1), cos_wide, sin_wide,
        np.ascontiguousarray(cosine.T), np.ascontiguousarray(sine.T),
        queries, out_grad, key_whole, value_whole,
    )


def finish(comp_total, rot_total, raw_latent, kv_gain, cosine, sine):
    inverse = lax.rsqrt(jnp.mean(raw_latent * raw_latent, axis=-1, keepdims=True) + norm_eps)
    mixed = comp_total * kv_gain
    spread = jnp.mean(raw_latent * mixed, axis=-1, keepdims=True)
    latent_grad = (inverse * mixed - raw_latent * inverse**3 * spread).astype(jnp.bfloat16)
    a, b = rot_total[:, :32], rot_total[:, 32:]
    rope_grad = jnp.concatenate([a * cosine + b * sine, b * cosine - a * sine], axis=-1)
    return latent_grad, rope_grad.astype(jnp.bfloat16)


def shards(queries, out_grad, latent, rope_key, kv_gain, key_up, value_up):
    ups = lax.all_gather(jnp.stack([key_up, value_up]), "dp", axis=1, tiled=True)
    length = latent.shape[1]
    grad_scale = float(lax.axis_size("dp") * length) ** (-0.5)
    query_grad, dw, part, rot = attention(
        queries[0], out_grad[0], latent[0], rope_key[0], kv_gain, ups[0], ups[1], grad_scale
    )
    dw = lax.psum_scatter(dw, "dp", scatter_dimension=1, tiled=True).astype(jnp.float32)
    comp_total = lax.psum(part, "sp").astype(jnp.float32)
    rot_total = lax.psum(rot, "sp").astype(jnp.float32)
    cosine, sine = rope_tables(length)
    latent_grad, rope_grad = finish(
        comp_total, rot_total, latent[0].astype(jnp.float32), kv_gain, cosine, sine
    )
    return query_grad[None], latent_grad[None], rope_grad[None], dw[0], dw[1]


def solution(mesh):
    return jax.shard_map(
        shards,
        mesh=mesh,
        in_specs=(
            P("dp", None, "sp"),
            P("dp", None, "sp"),
            P("dp", None, None),
            P("dp", None, None),
            P(),
            P("dp", "sp"),
            P("dp", "sp"),
        ),
        out_specs=(
            P("dp", None, "sp"),
            P("dp", None, None),
            P("dp", None, None),
            P("dp", "sp"),
            P("dp", "sp"),
        ),
        check_vma=False,
    )
```

```python
import functools

import jax
import jax.numpy as jnp
import numpy as np
from jax import lax
from jax.experimental import pallas as pl
from jax.experimental.pallas import tpu as pltpu
from jax.sharding import PartitionSpec as P

NOPE_DIM = 128
ROPE_DIM = 64
VALUE_DIM = 128
QK = NOPE_DIM + ROPE_DIM
LOG2E = 1.4426950408889634

norm_eps = 1e-06
rope_theta = 10000.0

NT = (((1,), (1,)), ((), ()))


def rope_tables(length):
    half = ROPE_DIM // 2
    frequency = np.float32(rope_theta) ** (-(np.arange(half, dtype=np.float32) * np.float32(2.0 / ROPE_DIM)))
    angles = np.arange(length, dtype=np.float32)[:, None] * frequency.astype(np.float32)[None, :]
    return np.cos(angles).astype(np.float32), np.sin(angles).astype(np.float32)


def dot(a, b):
    return jnp.dot(a, b, preferred_element_type=jnp.float32)


def dot_nt(a, b):
    return lax.dot_general(a, b, NT, preferred_element_type=jnp.float32)


def swap_halves(x):
    lane = lax.broadcasted_iota(jnp.int32, x.shape, 1)
    return jnp.where(lane % ROPE_DIM < ROPE_DIM // 2, pltpu.roll(x, 96, 1), pltpu.roll(x, 32, 1))


def attention_kernel(
    block, grad_scale,
    latent_ref, rope_ref, gain_ref, cos_ref, sin_ref, cos_t_ref, sin_t_ref,
    q_ref, do_ref, wk_ref, wv_ref,
    dq_ref, dw_ref, part_ref,
    comp, comp_t, krot, krot_t, ku, kt, vals, qu, pt, dst, dkv, acc, rot_acc,
):
    step = pl.program_id(0)
    length = q_ref.shape[0]
    tiles = length // block
    scale = QK ** (-0.5)

    @pl.when(step == 0)
    def _():
        raw = latent_ref[...].astype(jnp.float32)
        inverse = lax.rsqrt(jnp.mean(raw * raw, axis=-1, keepdims=True) + norm_eps)
        normed = raw * inverse * gain_ref[...]
        comp[...] = normed.astype(jnp.bfloat16)
        comp_t[...] = normed.T.astype(jnp.bfloat16)
        rope = rope_ref[...].astype(jnp.float32)
        wide = jnp.concatenate([rope, rope], axis=1)
        turned = wide * cos_ref[...] + swap_halves(wide) * sin_ref[...]
        krot[...] = turned.astype(jnp.bfloat16)
        krot_t[...] = turned.T.astype(jnp.bfloat16)
        acc[...] = jnp.zeros_like(acc)
        rot_acc[...] = jnp.zeros_like(rot_acc)

    keys = dot(comp[...], wk_ref[...])
    keys_t = keys.T.astype(jnp.bfloat16)
    keys = keys.astype(jnp.bfloat16)
    vals[...] = dot(comp[...], wv_ref[...]).astype(jnp.bfloat16)
    for h in range(2):
        ku[h, :, :NOPE_DIM] = keys[:, h * NOPE_DIM:(h + 1) * NOPE_DIM]
        ku[h, :, NOPE_DIM:] = krot[:, :ROPE_DIM]
        kt[h, :NOPE_DIM, :] = keys_t[h * NOPE_DIM:(h + 1) * NOPE_DIM, :]
        kt[h, NOPE_DIM:, :] = krot_t[:ROPE_DIM, :]

    mid = q_ref[:, 128:256].astype(jnp.float32)
    last = q_ref[:, 256:384].astype(jnp.float32)
    low = lax.broadcasted_iota(jnp.int32, mid.shape, 1) < 64
    plain = jnp.where(low, pltpu.roll(mid, 64, 1), pltpu.roll(last, 64, 1))
    rope = jnp.where(low, mid, last)
    turned = rope * cos_ref[...] + swap_halves(rope) * sin_ref[...]
    qu[0, :, :NOPE_DIM] = q_ref[:, :128]
    qu[0, :, NOPE_DIM:] = turned[:, :ROPE_DIM].astype(jnp.bfloat16)
    qu[1, :, :NOPE_DIM] = plain.astype(jnp.bfloat16)
    qu[1, :, NOPE_DIM:] = pltpu.roll(turned, 64, 1)[:, :ROPE_DIM].astype(jnp.bfloat16)

    for i in range(tiles):
        rows = slice(i * block, (i + 1) * block)
        n = (i + 1) * block
        parts = []
        for h in range(2):
            cols = slice(h * VALUE_DIM, (h + 1) * VALUE_DIM)
            scores = dot_nt(ku[h, :n, :], qu[h, rows, :])
            key_at = lax.broadcasted_iota(jnp.int32, (block, block), 0)
            query_at = lax.broadcasted_iota(jnp.int32, (block, block), 1)
            diag = jnp.where(key_at <= query_at, scores[n - block:], -jnp.inf)
            scores = diag if i == 0 else jnp.concatenate([scores[:n - block], diag], axis=0)
            top = jnp.max(scores, axis=0, keepdims=True)
            e = jnp.exp2((scores - top) * (scale * LOG2E))
            r = 1.0 / jnp.sum(e, axis=0, keepdims=True)
            prob_grad = dot_nt(vals[:n, cols], do_ref[rows, cols])
            center = jnp.sum(e * prob_grad, axis=0, keepdims=True) * r
            pt[h, :n, rows] = (e * r).astype(jnp.bfloat16)
            ds = (e * (r * scale) * (prob_grad - center)).astype(jnp.bfloat16)
            dst[h, :n, rows] = ds
            g = dot(kt[h, :, :n], ds)
            a = g[NOPE_DIM:NOPE_DIM + 32]
            b = g[NOPE_DIM + 32:]
            c, s = cos_t_ref[:, rows], sin_t_ref[:, rows]
            parts += [g[:NOPE_DIM], a * c + b * s, b * c - a * s]
        dq_ref[rows, :] = jnp.concatenate(parts, axis=0).T.astype(jnp.bfloat16)

    for h in range(2):
        for j in range(tiles):
            rows = slice(j * block, (j + 1) * block)
            cols = slice(h * VALUE_DIM, (h + 1) * VALUE_DIM)
            dv = dot(pt[h, rows, j * block:], do_ref[j * block:, cols])
            dk = dot(dst[h, rows, j * block:], qu[h, j * block:, :])
            dkv[rows, h * NOPE_DIM:(h + 1) * NOPE_DIM] = dk[:, :NOPE_DIM].astype(jnp.bfloat16)
            dkv[rows, (2 + h) * 128:(3 + h) * 128] = dv.astype(jnp.bfloat16)
            rot_acc[rows, :] += dk[:, NOPE_DIM:]

    dw = dot(comp_t[...], dkv[...]) * grad_scale
    dw_ref[:, 0] = dw[:, :256].reshape(dw_ref.shape[0], dw_ref.shape[2], 256).astype(dw_ref.dtype)
    dw_ref[:, 1] = dw[:, 256:].reshape(dw_ref.shape[0], dw_ref.shape[2], 256).astype(dw_ref.dtype)
    acc[...] += dot_nt(dkv[:, :256], wk_ref[...]) + dot_nt(dkv[:, 256:], wv_ref[...])

    @pl.when(step == pl.num_programs(0) - 1)
    def _():
        width = acc.shape[1]
        rot = rot_acc[...].astype(jnp.bfloat16)
        part_ref[:, :width] = acc[...].astype(jnp.bfloat16)
        part_ref[:, width:] = jnp.concatenate([rot, rot], axis=1)


def attention(queries, out_grad, latent, rope_key, kv_gain, key_whole, value_whole, grad_scale, n_dp):
    length = queries.shape[0]
    width = latent.shape[1]
    pairs = key_whole.shape[1] // 256
    block = 256
    cosine, sine = rope_tables(length)
    cos_wide = np.tile(cosine, (1, 4))
    sin_wide = np.concatenate([-sine, sine, -sine, sine], axis=1)
    bf, f32 = jnp.bfloat16, jnp.float32
    whole = lambda shape: pl.BlockSpec(shape, lambda p: (0,) * len(shape))
    column = lambda rows, cols: pl.BlockSpec((rows, cols), lambda p: (0, p))
    return pl.pallas_call(
        functools.partial(attention_kernel, block, grad_scale),
        grid=(pairs,),
        in_specs=[
            whole((length, width)), whole((length, ROPE_DIM)), whole((1, width)),
            whole((length, 128)), whole((length, 128)),
            whole((32, length)), whole((32, length)),
            column(length, 2 * QK), column(length, 256), column(width, 256), column(width, 256),
        ],
        out_specs=[
            column(length, 2 * QK),
            pl.BlockSpec((n_dp, 2, width // n_dp, 256), lambda p: (0, 0, 0, p)),
            whole((length, width + 128)),
        ],
        out_shape=[
            jax.ShapeDtypeStruct(queries.shape, bf),
            jax.ShapeDtypeStruct((n_dp, 2, width // n_dp, key_whole.shape[1]), bf),
            jax.ShapeDtypeStruct((length, width + 128), bf),
        ],
        scratch_shapes=[
            pltpu.VMEM((length, width), bf), pltpu.VMEM((width, length), bf),
            pltpu.VMEM((length, 128), bf), pltpu.VMEM((128, length), bf),
            pltpu.VMEM((2, length, QK), bf), pltpu.VMEM((2, QK, length), bf),
            pltpu.VMEM((length, 256), bf), pltpu.VMEM((2, length, QK), bf),
            pltpu.VMEM((2, length, length), bf), pltpu.VMEM((2, length, length), bf),
            pltpu.VMEM((length, 512), bf),
            pltpu.VMEM((length, width), f32), pltpu.VMEM((length, ROPE_DIM), f32),
        ],
        compiler_params=pltpu.CompilerParams(
            dimension_semantics=("arbitrary",), vmem_limit_bytes=48 * 1024 * 1024
        ),
        cost_estimate=pl.CostEstimate(flops=10_000_000_000, bytes_accessed=12_000_000, transcendentals=4_000_000),
        name="attention_backward",
    )(
        latent, rope_key, kv_gain.reshape(1, -1), cos_wide, sin_wide,
        np.ascontiguousarray(cosine.T), np.ascontiguousarray(sine.T),
        queries, out_grad, key_whole, value_whole,
    )


def exchange_kernel(
    n_sp, n_dp,
    dw_ref, part_ref, latent_ref, gain_ref, cos_ref, sin_ref,
    grad_ref, low_ref,
    got_part, got_dw, send_a, recv_a, send_b, recv_b, send_c, recv_c,
):
    sp, dp = lax.axis_index("sp"), lax.axis_index("dp")
    rows = latent_ref.shape[0] // n_sp
    width = latent_ref.shape[1]
    mine = pl.ds(pl.multiple_of(sp * rows, rows), rows)
    mesh_id = pl.DeviceIdType.MESH
    barrier = pltpu.get_barrier_semaphore()

    def each(count, act):
        def body(k, carry):
            act(k)
            return carry
        lax.fori_loop(1, count, body, 0)

    def greet(axis, here, count):
        each(count, lambda k: pl.semaphore_signal(
            barrier, inc=1, device_id={axis: lax.rem(here + k, count)}, device_id_type=mesh_id))

    greet("sp", sp, n_sp)
    greet("dp", dp, n_dp)
    pl.semaphore_wait(barrier, n_sp + n_dp - 2)

    def part_copy(k):
        peer = lax.rem(sp + k, n_sp)
        return pltpu.make_async_remote_copy(
            src_ref=part_ref.at[pl.ds(pl.multiple_of(peer * rows, rows), rows)],
            dst_ref=got_part.at[k], send_sem=send_a.at[k], recv_sem=recv_a.at[k],
            device_id={"sp": peer}, device_id_type=mesh_id)

    def dw_copy(k):
        peer = lax.rem(dp + k, n_dp)
        return pltpu.make_async_remote_copy(
            src_ref=dw_ref.at[peer], dst_ref=got_dw.at[k],
            send_sem=send_b.at[k], recv_sem=recv_b.at[k],
            device_id={"dp": peer}, device_id_type=mesh_id)

    def low_copy(k):
        return pltpu.make_async_remote_copy(
            src_ref=low_ref.at[mine], dst_ref=low_ref.at[mine],
            send_sem=send_c.at[k], recv_sem=recv_c.at[k],
            device_id={"sp": lax.rem(sp + k, n_sp)}, device_id_type=mesh_id)

    each(n_sp, lambda k: part_copy(k).start())
    each(n_dp, lambda k: dw_copy(k).start())

    total = part_ref[mine, :].astype(jnp.float32)
    each(n_sp, lambda k: part_copy(k).wait())
    for k in range(1, n_sp):
        total = total + got_part[k].astype(jnp.float32)
    raw = latent_ref[mine, :].astype(jnp.float32)
    inverse = lax.rsqrt(jnp.mean(raw * raw, axis=-1, keepdims=True) + norm_eps)
    mixed = total[:, :width] * gain_ref[...]
    spread = jnp.mean(raw * mixed, axis=-1, keepdims=True)
    low_ref[mine, :width] = (inverse * mixed - raw * inverse**3 * spread).astype(jnp.bfloat16)
    rot = total[:, width:]
    low_ref[mine, width:] = (
        rot * cos_ref[mine, :] - swap_halves(rot) * sin_ref[mine, :]
    ).astype(jnp.bfloat16)
    each(n_sp, lambda k: low_copy(k).start())

    grad_ref[...] = dw_ref[dp].astype(jnp.float32)
    def add(k):
        dw_copy(k).wait()
        grad_ref[...] += got_dw[k].astype(jnp.float32)
    each(n_dp, add)
    each(n_sp, lambda k: low_copy(k).wait())


def exchange(dw, part, latent, kv_gain, n_sp, n_dp):
    length, width = latent.shape
    cosine, sine = rope_tables(length)
    bf = jnp.bfloat16
    vmem = pl.BlockSpec(memory_space=pltpu.VMEM)
    sems = lambda n: pltpu.SemaphoreType.DMA((n,))
    return pl.pallas_call(
        functools.partial(exchange_kernel, n_sp, n_dp),
        in_specs=[vmem] * 6,
        out_specs=[vmem] * 2,
        out_shape=[
            jax.ShapeDtypeStruct(dw.shape[1:], jnp.float32),
            jax.ShapeDtypeStruct(part.shape, bf),
        ],
        scratch_shapes=[
            pltpu.VMEM((n_sp, length // n_sp, part.shape[1]), bf),
            pltpu.VMEM(dw.shape, bf),
            sems(n_sp), sems(n_sp), sems(n_dp), sems(n_dp), sems(n_sp), sems(n_sp),
        ],
        compiler_params=pltpu.CompilerParams(
            collective_id=0, has_side_effects=True, vmem_limit_bytes=32 * 1024 * 1024
        ),
        name="exchange",
    )(
        dw, part, latent, kv_gain.reshape(1, -1), np.tile(cosine, (1, 4)),
        np.concatenate([-sine, sine, -sine, sine], axis=1),
    )


def shards(queries, out_grad, latent, rope_key, kv_gain, key_up, value_up):
    ups = lax.all_gather(jnp.stack([key_up, value_up]), "dp", axis=1, tiled=True)
    length, width = latent.shape[1:]
    n_sp, n_dp = lax.axis_size("sp"), lax.axis_size("dp")
    grad_scale = float(n_dp * length) ** (-0.5)
    query_grad, dw, part = attention(
        queries[0], out_grad[0], latent[0], rope_key[0], kv_gain, ups[0], ups[1], grad_scale, n_dp
    )
    dw, low = exchange(dw, part, latent[0], kv_gain, n_sp, n_dp)
    return query_grad[None], low[None, :, :width], low[None, :, width:width + ROPE_DIM], dw[0], dw[1]


def solution(mesh):
    return jax.shard_map(
        shards,
        mesh=mesh,
        in_specs=(
            P("dp", None, "sp"),
            P("dp", None, "sp"),
            P("dp", None, None),
            P("dp", None, None),
            P(),
            P("dp", "sp"),
            P("dp", "sp"),
        ),
        out_specs=(
            P("dp", None, "sp"),
            P("dp", None, None),
            P("dp", None, None),
            P("dp", "sp"),
            P("dp", "sp"),
        ),
        check_vma=False,
    )
```

```python
import functools

import jax
import jax.numpy as jnp
import numpy as np
from jax import lax
from jax.experimental import pallas as pl
from jax.experimental.pallas import tpu as pltpu
from jax.sharding import PartitionSpec as P

NOPE_DIM = 128
ROPE_DIM = 64
VALUE_DIM = 128
QK = NOPE_DIM + ROPE_DIM
LOG2E = 1.4426950408889634

norm_eps = 1e-06
rope_theta = 10000.0

NT = (((1,), (1,)), ((), ()))


def rope_tables(length):
    half = ROPE_DIM // 2
    frequency = np.float32(rope_theta) ** (-(np.arange(half, dtype=np.float32) * np.float32(2.0 / ROPE_DIM)))
    angles = np.arange(length, dtype=np.float32)[:, None] * frequency.astype(np.float32)[None, :]
    return np.cos(angles).astype(np.float32), np.sin(angles).astype(np.float32)


def dot(a, b):
    return jnp.dot(a, b, preferred_element_type=jnp.float32)


def dot_nt(a, b):
    return lax.dot_general(a, b, NT, preferred_element_type=jnp.float32)


def swap_halves(x):
    lane = lax.broadcasted_iota(jnp.int32, x.shape, 1)
    return jnp.where(lane % ROPE_DIM < ROPE_DIM // 2, pltpu.roll(x, 96, 1), pltpu.roll(x, 32, 1))


def attention_kernel(
    block, grad_scale,
    latent_ref, rope_ref, gain_ref, cos_ref, sin_ref, cos_t_ref, sin_t_ref,
    q_ref, do_ref, wk_ref, wv_ref,
    dq_ref, dw_ref, part_ref,
    comp, comp_t, krot, krot_t, ku, kt, vals, qu, pt, dst, dkv, acc, rot_acc,
):
    step = pl.program_id(0)
    length = q_ref.shape[0]
    tiles = length // block
    scale = QK ** (-0.5)

    @pl.when(step == 0)
    def _():
        raw = latent_ref[...].astype(jnp.float32)
        inverse = lax.rsqrt(jnp.mean(raw * raw, axis=-1, keepdims=True) + norm_eps)
        normed = raw * inverse * gain_ref[...]
        comp[...] = normed.astype(jnp.bfloat16)
        comp_t[...] = normed.T.astype(jnp.bfloat16)
        rope = rope_ref[...].astype(jnp.float32)
        wide = jnp.concatenate([rope, rope], axis=1)
        turned = wide * cos_ref[...] + swap_halves(wide) * sin_ref[...]
        krot[...] = turned.astype(jnp.bfloat16)
        krot_t[...] = turned.T.astype(jnp.bfloat16)
        acc[...] = jnp.zeros_like(acc)
        rot_acc[...] = jnp.zeros_like(rot_acc)

    keys = dot(comp[...], wk_ref[...])
    keys_t = keys.T.astype(jnp.bfloat16)
    keys = keys.astype(jnp.bfloat16)
    vals[...] = dot(comp[...], wv_ref[...]).astype(jnp.bfloat16)
    for h in range(2):
        ku[h, :, :NOPE_DIM] = keys[:, h * NOPE_DIM:(h + 1) * NOPE_DIM]
        ku[h, :, NOPE_DIM:] = krot[:, :ROPE_DIM]
        kt[h, :NOPE_DIM, :] = keys_t[h * NOPE_DIM:(h + 1) * NOPE_DIM, :]
        kt[h, NOPE_DIM:, :] = krot_t[:ROPE_DIM, :]

    mid = q_ref[:, 128:256].astype(jnp.float32)
    last = q_ref[:, 256:384].astype(jnp.float32)
    low = lax.broadcasted_iota(jnp.int32, mid.shape, 1) < 64
    plain = jnp.where(low, pltpu.roll(mid, 64, 1), pltpu.roll(last, 64, 1))
    rope = jnp.where(low, mid, last)
    turned = rope * cos_ref[...] + swap_halves(rope) * sin_ref[...]
    qu[0, :, :NOPE_DIM] = q_ref[:, :128]
    qu[0, :, NOPE_DIM:] = turned[:, :ROPE_DIM].astype(jnp.bfloat16)
    qu[1, :, :NOPE_DIM] = plain.astype(jnp.bfloat16)
    qu[1, :, NOPE_DIM:] = pltpu.roll(turned, 64, 1)[:, :ROPE_DIM].astype(jnp.bfloat16)

    for i in range(tiles):
        rows = slice(i * block, (i + 1) * block)
        n = (i + 1) * block
        parts = []
        for h in range(2):
            cols = slice(h * VALUE_DIM, (h + 1) * VALUE_DIM)
            scores = dot_nt(ku[h, :n, :], qu[h, rows, :])
            key_at = lax.broadcasted_iota(jnp.int32, (block, block), 0)
            query_at = lax.broadcasted_iota(jnp.int32, (block, block), 1)
            diag = jnp.where(key_at <= query_at, scores[n - block:], -jnp.inf)
            scores = diag if i == 0 else jnp.concatenate([scores[:n - block], diag], axis=0)
            top = jnp.max(scores, axis=0, keepdims=True)
            e = jnp.exp2((scores - top) * (scale * LOG2E))
            r = 1.0 / jnp.sum(e, axis=0, keepdims=True)
            prob_grad = dot_nt(vals[:n, cols], do_ref[rows, cols])
            center = jnp.sum(e * prob_grad, axis=0, keepdims=True) * r
            pt[h, :n, rows] = (e * r).astype(jnp.bfloat16)
            ds = (e * (r * scale) * (prob_grad - center)).astype(jnp.bfloat16)
            dst[h, :n, rows] = ds
            g = dot(kt[h, :, :n], ds)
            a = g[NOPE_DIM:NOPE_DIM + 32]
            b = g[NOPE_DIM + 32:]
            c, s = cos_t_ref[:, rows], sin_t_ref[:, rows]
            parts += [g[:NOPE_DIM], a * c + b * s, b * c - a * s]
        dq_ref[rows, :] = jnp.concatenate(parts, axis=0).T.astype(jnp.bfloat16)

    for h in range(2):
        for j in range(tiles):
            rows = slice(j * block, (j + 1) * block)
            cols = slice(h * VALUE_DIM, (h + 1) * VALUE_DIM)
            dv = dot(pt[h, rows, j * block:], do_ref[j * block:, cols])
            dk = dot(dst[h, rows, j * block:], qu[h, j * block:, :])
            dkv[rows, h * NOPE_DIM:(h + 1) * NOPE_DIM] = dk[:, :NOPE_DIM].astype(jnp.bfloat16)
            dkv[rows, (2 + h) * 128:(3 + h) * 128] = dv.astype(jnp.bfloat16)
            rot_acc[rows, :] += dk[:, NOPE_DIM:]

    dw = dot(comp_t[...], dkv[...]) * grad_scale
    dw_ref[:, 0] = dw[:, :256].reshape(dw_ref.shape[0], dw_ref.shape[2], 256).astype(dw_ref.dtype)
    dw_ref[:, 1] = dw[:, 256:].reshape(dw_ref.shape[0], dw_ref.shape[2], 256).astype(dw_ref.dtype)
    acc[...] += dot_nt(dkv[:, :256], wk_ref[...]) + dot_nt(dkv[:, 256:], wv_ref[...])

    @pl.when(step == pl.num_programs(0) - 1)
    def _():
        width = acc.shape[1]
        rot = rot_acc[...].astype(jnp.bfloat16)
        part_ref[:, :width] = acc[...].astype(jnp.bfloat16)
        part_ref[:, width:] = jnp.concatenate([rot, rot], axis=1)


def attention(queries, out_grad, latent, rope_key, kv_gain, key_whole, value_whole, grad_scale, n_dp):
    length = queries.shape[0]
    width = latent.shape[1]
    pairs = key_whole.shape[1] // 256
    block = 256
    cosine, sine = rope_tables(length)
    cos_wide = np.tile(cosine, (1, 4))
    sin_wide = np.concatenate([-sine, sine, -sine, sine], axis=1)
    bf, f32 = jnp.bfloat16, jnp.float32
    whole = lambda shape: pl.BlockSpec(shape, lambda p: (0,) * len(shape))
    column = lambda rows, cols: pl.BlockSpec((rows, cols), lambda p: (0, p))
    return pl.pallas_call(
        functools.partial(attention_kernel, block, grad_scale),
        grid=(pairs,),
        in_specs=[
            whole((length, width)), whole((length, ROPE_DIM)), whole((1, width)),
            whole((length, 128)), whole((length, 128)),
            whole((32, length)), whole((32, length)),
            column(length, 2 * QK), column(length, 256), column(width, 256), column(width, 256),
        ],
        out_specs=[
            column(length, 2 * QK),
            pl.BlockSpec((n_dp, 2, width // n_dp, 256), lambda p: (0, 0, 0, p)),
            whole((length, width + 128)),
        ],
        out_shape=[
            jax.ShapeDtypeStruct(queries.shape, bf),
            jax.ShapeDtypeStruct((n_dp, 2, width // n_dp, key_whole.shape[1]), bf),
            jax.ShapeDtypeStruct((length, width + 128), bf),
        ],
        scratch_shapes=[
            pltpu.VMEM((length, width), bf), pltpu.VMEM((width, length), bf),
            pltpu.VMEM((length, 128), bf), pltpu.VMEM((128, length), bf),
            pltpu.VMEM((2, length, QK), bf), pltpu.VMEM((2, QK, length), bf),
            pltpu.VMEM((length, 256), bf), pltpu.VMEM((2, length, QK), bf),
            pltpu.VMEM((2, length, length), bf), pltpu.VMEM((2, length, length), bf),
            pltpu.VMEM((length, 512), bf),
            pltpu.VMEM((length, width), f32), pltpu.VMEM((length, ROPE_DIM), f32),
        ],
        compiler_params=pltpu.CompilerParams(
            dimension_semantics=("arbitrary",), vmem_limit_bytes=48 * 1024 * 1024
        ),
        cost_estimate=pl.CostEstimate(flops=10_000_000_000, bytes_accessed=12_000_000, transcendentals=4_000_000),
        name="attention_backward",
    )(
        latent, rope_key, kv_gain.reshape(1, -1), cos_wide, sin_wide,
        np.ascontiguousarray(cosine.T), np.ascontiguousarray(sine.T),
        queries, out_grad, key_whole, value_whole,
    )


def exchange_kernel(
    n_sp, n_dp,
    dw_ref, part_ref, latent_ref, gain_ref, cos_ref, sin_ref,
    grad_ref, low_ref,
    got_part, got_dw, send_a, recv_a, send_b, recv_b, send_c, recv_c,
):
    sp, dp = lax.axis_index("sp"), lax.axis_index("dp")
    rows = latent_ref.shape[0] // n_sp
    width = latent_ref.shape[1]
    mine = pl.ds(pl.multiple_of(sp * rows, rows), rows)
    mesh_id = pl.DeviceIdType.MESH
    barrier = pltpu.get_barrier_semaphore()

    def each(count, act):
        def body(k, carry):
            act(k)
            return carry
        lax.fori_loop(1, count, body, 0)

    def greet(axis, here, count):
        each(count, lambda k: pl.semaphore_signal(
            barrier, inc=1, device_id={axis: lax.rem(here + k, count)}, device_id_type=mesh_id))

    greet("sp", sp, n_sp)
    greet("dp", dp, n_dp)
    pl.semaphore_wait(barrier, n_sp + n_dp - 2)

    def part_copy(k):
        peer = lax.rem(sp + k, n_sp)
        return pltpu.make_async_remote_copy(
            src_ref=part_ref.at[pl.ds(pl.multiple_of(peer * rows, rows), rows)],
            dst_ref=got_part.at[k], send_sem=send_a.at[k], recv_sem=recv_a.at[k],
            device_id={"sp": peer}, device_id_type=mesh_id)

    def dw_copy(k):
        peer = lax.rem(dp + k, n_dp)
        return pltpu.make_async_remote_copy(
            src_ref=dw_ref.at[peer], dst_ref=got_dw.at[k],
            send_sem=send_b.at[k], recv_sem=recv_b.at[k],
            device_id={"dp": peer}, device_id_type=mesh_id)

    def low_copy(k):
        return pltpu.make_async_remote_copy(
            src_ref=low_ref.at[mine], dst_ref=low_ref.at[mine],
            send_sem=send_c.at[k], recv_sem=recv_c.at[k],
            device_id={"sp": lax.rem(sp + k, n_sp)}, device_id_type=mesh_id)

    each(n_sp, lambda k: part_copy(k).start())
    each(n_dp, lambda k: dw_copy(k).start())

    total = part_ref[mine, :].astype(jnp.float32)
    each(n_sp, lambda k: part_copy(k).wait())
    for k in range(1, n_sp):
        total = total + got_part[k].astype(jnp.float32)
    raw = latent_ref[mine, :].astype(jnp.float32)
    inverse = lax.rsqrt(jnp.mean(raw * raw, axis=-1, keepdims=True) + norm_eps)
    mixed = total[:, :width] * gain_ref[...]
    spread = jnp.mean(raw * mixed, axis=-1, keepdims=True)
    low_ref[mine, :width] = (inverse * mixed - raw * inverse**3 * spread).astype(jnp.bfloat16)
    rot = total[:, width:]
    low_ref[mine, width:] = (
        rot * cos_ref[mine, :] - swap_halves(rot) * sin_ref[mine, :]
    ).astype(jnp.bfloat16)
    each(n_sp, lambda k: low_copy(k).start())

    grad_ref[...] = dw_ref[dp].astype(jnp.float32)
    def add(k):
        dw_copy(k).wait()
        grad_ref[...] += got_dw[k].astype(jnp.float32)
    each(n_dp, add)
    each(n_sp, lambda k: low_copy(k).wait())


def exchange(dw, part, latent, kv_gain, n_sp, n_dp):
    length, width = latent.shape
    cosine, sine = rope_tables(length)
    bf = jnp.bfloat16
    vmem = pl.BlockSpec(memory_space=pltpu.VMEM)
    sems = lambda n: pltpu.SemaphoreType.DMA((n,))
    return pl.pallas_call(
        functools.partial(exchange_kernel, n_sp, n_dp),
        in_specs=[vmem] * 6,
        out_specs=[vmem] * 2,
        out_shape=[
            jax.ShapeDtypeStruct(dw.shape[1:], jnp.float32),
            jax.ShapeDtypeStruct(part.shape, bf),
        ],
        scratch_shapes=[
            pltpu.VMEM((n_sp, length // n_sp, part.shape[1]), bf),
            pltpu.VMEM(dw.shape, bf),
            sems(n_sp), sems(n_sp), sems(n_dp), sems(n_dp), sems(n_sp), sems(n_sp),
        ],
        compiler_params=pltpu.CompilerParams(
            collective_id=0, has_side_effects=True, vmem_limit_bytes=32 * 1024 * 1024
        ),
        name="exchange",
    )(
        dw, part, latent, kv_gain.reshape(1, -1), np.tile(cosine, (1, 4)),
        np.concatenate([-sine, sine, -sine, sine], axis=1),
    )


def gather_kernel(
    n_dp, key_ref, value_ref, key_out, value_out, send_a, recv_a, send_b, recv_b
):
    dp = lax.axis_index("dp")
    chips = n_dp // 2
    chip, core = dp // 2, lax.rem(dp, 2)
    partner = chip * 2 + 1 - core
    mesh_id = pl.DeviceIdType.MESH
    barrier = pltpu.get_barrier_semaphore()
    pairs = ((key_ref, key_out), (value_ref, value_out))

    def each(act):
        def body(k, carry):
            act(k)
            return carry
        lax.fori_loop(1, chips, body, 0)

    def other(k):
        return lax.rem(chip + k, chips) * 2 + core

    def source(k):
        return lax.rem(chip - k + chips, chips) * 2 + core

    each(lambda k: pl.semaphore_signal(
        barrier, inc=1, device_id={"dp": other(k)}, device_id_type=mesh_id))
    pl.semaphore_signal(barrier, inc=1, device_id={"dp": partner}, device_id_type=mesh_id)
    pl.semaphore_wait(barrier, chips)

    def far(t, k):
        return pltpu.make_async_remote_copy(
            src_ref=pairs[t][0], dst_ref=pairs[t][1].at[dp],
            send_sem=send_a.at[t, k], recv_sem=recv_a.at[t, k],
            device_id={"dp": other(k)}, device_id_type=mesh_id)

    def near(t, k, own):
        block = dp if own else source(k)
        return pltpu.make_async_remote_copy(
            src_ref=pairs[t][0] if own else pairs[t][1].at[block],
            dst_ref=pairs[t][1].at[block],
            send_sem=send_b.at[t, k], recv_sem=recv_b.at[t, k],
            device_id={"dp": partner}, device_id_type=mesh_id)

    for t in range(2):
        each(lambda k: far(t, k).start())
    for t in range(2):
        near(t, 0, True).start()
        pairs[t][1][dp] = pairs[t][0][...]

    def forward(k):
        for t in range(2):
            far(t, k).wait_recv()
            near(t, k, False).start()

    def drain(k):
        for t in range(2):
            far(t, k).wait_send()
            near(t, k, False).wait()

    each(forward)
    for t in range(2):
        near(t, 0, True).wait()
    each(drain)


def gather(key_up, value_up, n_dp):
    vmem = pl.BlockSpec(memory_space=pltpu.VMEM)
    shape = jax.ShapeDtypeStruct((n_dp, *key_up.shape), key_up.dtype)
    outs = pl.pallas_call(
        functools.partial(gather_kernel, n_dp),
        in_specs=[vmem] * 2,
        out_specs=[vmem] * 2,
        out_shape=[shape, shape],
        scratch_shapes=[pltpu.SemaphoreType.DMA((2, n_dp // 2))] * 4,
        compiler_params=pltpu.CompilerParams(
            collective_id=1, has_side_effects=True, vmem_limit_bytes=16 * 1024 * 1024
        ),
        name="gather",
    )(key_up, value_up)
    return [out.reshape(n_dp * key_up.shape[0], -1) for out in outs]


def shards(queries, out_grad, latent, rope_key, kv_gain, key_up, value_up):
    length, width = latent.shape[1:]
    n_sp, n_dp = lax.axis_size("sp"), lax.axis_size("dp")
    grad_scale = float(n_dp * length) ** (-0.5)
    key_whole, value_whole = gather(key_up, value_up, n_dp)
    query_grad, dw, part = attention(
        queries[0], out_grad[0], latent[0], rope_key[0], kv_gain, key_whole, value_whole, grad_scale, n_dp
    )
    dw, low = exchange(dw, part, latent[0], kv_gain, n_sp, n_dp)
    return query_grad[None], low[None, :, :width], low[None, :, width:width + ROPE_DIM], dw[0], dw[1]


def solution(mesh):
    return jax.shard_map(
        shards,
        mesh=mesh,
        in_specs=(
            P("dp", None, "sp"),
            P("dp", None, "sp"),
            P("dp", None, None),
            P("dp", None, None),
            P(),
            P("dp", "sp"),
            P("dp", "sp"),
        ),
        out_specs=(
            P("dp", None, "sp"),
            P("dp", None, None),
            P("dp", None, None),
            P("dp", "sp"),
            P("dp", "sp"),
        ),
        check_vma=False,
    )
```
